32 devices in a mesh: grp: 2 (over y), ra: 4 (over z), cb: 4 (over x, core).
Axes of the slice: x: 2, y: 2, z: 4, core: 2. Of those that a mesh axis runs over, the one named last changes fastest.
Arguments:
- tokens: bfloat16 [256, 2048], P('grp', 'ra'), parts along dimension 0, may hold values from -8 to 8
- first_gain: bfloat16 [2048], P('ra'), may hold values from 0.099609375 to 1.8984375
- first_gate: bfloat16 [2048, 5632], P('ra', 'cb'), may hold values from -0.125 to 0.125
- first_up: bfloat16 [2048, 5632], P('ra', 'cb'), may hold values from -0.125 to 0.125
- first_down: bfloat16 [5632, 2048], P('cb', 'ra'), may hold values from -0.078125 to 0.078125
- second_gain: bfloat16 [2048], P('ra'), may hold values from 0.099609375 to 1.8984375
- second_gate: bfloat16 [2048, 5632], P('ra', 'cb'), may hold values from -0.125 to 0.125
- second_up: bfloat16 [2048, 5632], P('ra', 'cb'), may hold values from -0.125 to 0.125
- second_down: bfloat16 [5632, 2048], P('cb', 'ra'), may hold values from -0.078125 to 0.078125
Outputs:
- latent_out: bfloat16 [256, 2048], P('grp', 'ra'), parts along dimension 0
The draws below stay inside these ranges and needn't reach their ends.
There are 2 independent parts, one for each index of `grp`. The reference program is written for one: setup_inputs(seed, part) draws one part's arguments, and reference() takes and returns one part's arrays. A program takes and returns all parts, laid end to end along the dimension named above; an argument that names none is the same for every part. Nothing has to cross between parts.
All inputs are finite; a program needn't handle non-finite values.
Results may differ from the reference program's by a relative error of at most 0.0088.
Values may be sent and summed in bfloat16 or wider, within the bound.
No kernel may reach another device: no remote copies, remote signals or barrier semaphores. Data moves between devices by JAX's collectives and lax.ppermute only.
A program may use at most 64 MiB of HBM per device.

```python
import math
import jax
import jax.numpy as jnp
from jax import lax

D = 2048
FF = 5632
TOKENS = 128


def draw_tokens(key, part):
    keys = jax.random.split(jax.random.fold_in(key, 11), 3)
    row_scale = jnp.exp(jax.random.uniform(keys[0], (TOKENS, 1), jnp.float32, math.log(0.1), 0.0))
    ramp = jnp.exp(math.log(6.0) * jnp.arange(D, dtype=jnp.float32) / D) / 2.5
    col_scale = ramp * jnp.exp(jax.random.uniform(keys[1], (D,), jnp.float32, -0.35, 0.35))
    base = jax.random.normal(keys[2], (TOKENS, D), jnp.float32)
    return jnp.clip(base * row_scale * col_scale, -8.0, 8.0).astype(jnp.bfloat16)


def steps_of(rng, dims, cuts, smallest, largest):
    def one(axis_at, shards_of):
        heights = jax.random.uniform(jax.random.fold_in(jax.random.fold_in(rng, 6), axis_at), (shards_of,), jnp.float32, smallest / len(cuts), largest / len(cuts))
        return jnp.repeat(jnp.exp(heights), dims[axis_at] // shards_of).reshape((-1,) + (1,) * (len(dims) - axis_at - 1))

    factor_of = one(*cuts[0])
    for cut in cuts[1:]:
        factor_of = factor_of * one(*cut)
    return factor_of


def centred(key, extent, deviation, bound, shards=(), kind=jnp.bfloat16):
    level = steps_of(key, extent, shards, -0.22, 0.18) if shards else 1.0
    result = jax.random.normal(key, extent, jnp.float32) * deviation * level
    return jnp.minimum(jnp.maximum(result, -bound), bound).astype(kind)


def setup_inputs(seed: int = 0, part: int = 0) -> dict:
    key_of = jax.random.split(jax.random.key(seed), 10)
    part_keys = jax.random.split(jax.random.fold_in(key_of[9], part), 10)
    tokens = draw_tokens(jax.random.fold_in(jax.random.fold_in(key_of[9], part), 71), part)
    first_gain = jnp.clip(1.0 + 0.18 * jax.random.normal(key_of[1], (D,), jnp.float32), 0.099609375, 1.8984375).astype(jnp.bfloat16)
    first_gate = centred(key_of[2], (D, FF), D ** -0.5, 0.125, ((0, 4), (1, 4)))
    first_up = centred(key_of[3], (D, FF), D ** -0.5, 0.125, ((0, 4), (1, 4)))
    first_down = centred(key_of[4], (FF, D), FF ** -0.5, 0.078125, ((0, 4), (1, 4)))
    second_gain = jnp.clip(1.0 + 0.18 * jax.random.normal(key_of[5], (D,), jnp.float32), 0.099609375, 1.8984375).astype(jnp.bfloat16)
    second_gate = centred(key_of[6], (D, FF), D ** -0.5, 0.125, ((0, 4), (1, 4)))
    second_up = centred(key_of[7], (D, FF), D ** -0.5, 0.125, ((0, 4), (1, 4)))
    second_down = centred(key_of[8], (FF, D), FF ** -0.5, 0.078125, ((0, 4), (1, 4)))
    return {"tokens": tokens, "first_gain": first_gain, "first_gate": first_gate, "first_up": first_up, "first_down": first_down, "second_gain": second_gain, "second_gate": second_gate, "second_up": second_up, "second_down": second_down}


def sublayer(x, gain, w_gate, w_up, w_down):
    xf = x.astype(jnp.float32)
    scale = jax.lax.rsqrt(lax.optimization_barrier(jnp.mean(xf * xf, axis=1)) + 1e-06)
    normed = (xf * gain.astype(jnp.float32)).astype(jnp.bfloat16)
    gate_pre = scale[:, None] * jnp.dot(normed, w_gate, preferred_element_type=jnp.float32)
    up_pre = scale[:, None] * jnp.dot(normed, w_up, preferred_element_type=jnp.float32)
    hidden = (jax.nn.silu(gate_pre) * up_pre).astype(jnp.bfloat16)
    branch = jnp.dot(hidden, w_down, preferred_element_type=jnp.float32)
    return (0.5 * xf + 0.5 * branch).astype(jnp.bfloat16)

def reference(tokens, first_gain, first_gate, first_up, first_down, second_gain, second_gate, second_up, second_down):
    middle = sublayer(tokens, first_gain, first_gate, first_up, first_down)
    return sublayer(middle, second_gain, second_gate, second_up, second_down)
```

```python
import jax
import jax.numpy as jnp
from jax import lax
from jax.sharding import PartitionSpec as P

CHUNKS = 1
bf16, f32 = jnp.bfloat16, jnp.float32


def bits_of(axis):
    size, out, k = lax.axis_size(axis), [], 1
    while k < size:
        out.append(k)
        k *= 2
    assert k == size
    return out


def swap(x, axis, bit):
    return lax.ppermute(x, axis, [(i, i ^ bit) for i in range(lax.axis_size(axis))])


def local_order(x, axis):
    me, levels = lax.axis_index(axis), bits_of(axis)
    y = x.reshape((2,) * len(levels) + (-1, x.shape[1]))
    for dim, bit in enumerate(levels):
        y = jnp.where((me & bit) != 0, jnp.flip(y, dim), y)
    return y.reshape(x.shape)


def up_half(x, gain, w_gate, w_up):
    xf = x.astype(f32)
    squares = jnp.sum(xf * xf, axis=1, keepdims=True)
    high = squares.astype(bf16).astype(f32)
    normed = (xf * gain.astype(f32)).astype(bf16)
    gate = jnp.dot(normed, w_gate, preferred_element_type=f32)
    up = jnp.dot(normed, w_up, preferred_element_type=f32)
    lane = lax.broadcasted_iota(jnp.int32, (x.shape[0], 128), 1)
    sq = jnp.where(lane == 0, high, jnp.where(lane == 1, squares - high, 0.0))
    return jnp.concatenate([gate, up, sq], axis=1)


def sublayer(x, gain, w_gate, w_up, w_down):
    width = x.shape[1] * lax.axis_size("ra")
    ff = w_gate.shape[1]
    part = up_half(x, gain, w_gate, w_up)
    for bit in bits_of("ra"):
        half = part.shape[0] // 2
        part = part[:half] + swap(part[half:].astype(bf16), "ra", bit).astype(f32)
    total = part[:, 2 * ff : 2 * ff + 1] + part[:, 2 * ff + 1 : 2 * ff + 2]
    scale = lax.rsqrt(total / width + 1e-06)
    hidden = (jax.nn.silu(part[:, :ff] * scale) * (part[:, ff : 2 * ff] * scale)).astype(bf16)
    for bit in reversed(bits_of("ra")):
        hidden = jnp.concatenate([hidden, swap(hidden, "ra", bit)], axis=0)
    branch = jnp.dot(hidden, w_down, preferred_element_type=f32)
    for bit in bits_of("cb"):
        branch = branch + swap(branch.astype(bf16), "cb", bit).astype(f32)
    return (0.5 * x.astype(f32) + 0.5 * branch).astype(bf16)


def per_device(tokens, first_gain, first_gate, first_up, first_down, second_gain, second_gate, second_up, second_down):
    rows = tokens.shape[0] // CHUNKS
    outs = []
    for c in range(CHUNKS):
        x = local_order(tokens[c * rows : (c + 1) * rows], "ra")
        x = sublayer(x, first_gain, first_gate, first_up, first_down)
        x = sublayer(x, second_gain, second_gate, second_up, second_down)
        outs.append(local_order(x, "ra"))
    return jnp.concatenate(outs, axis=0)


def solution(mesh):
    placed = (
        P("grp", "ra"),
        P("ra"),
        P("ra", "cb"),
        P("ra", "cb"),
        P("cb", "ra"),
        P("ra"),
        P("ra", "cb"),
        P("ra", "cb"),
        P("cb", "ra"),
    )
    return jax.shard_map(
        per_device, mesh=mesh, in_specs=placed, out_specs=P("grp", "ra"), check_vma=False
    )
```

```python
import jax
import jax.numpy as jnp
from jax import lax
from jax.sharding import PartitionSpec as P

CHUNKS = 2
bf16, f32 = jnp.bfloat16, jnp.float32


def bits_of(axis):
    size, out, k = lax.axis_size(axis), [], 1
    while k < size:
        out.append(k)
        k *= 2
    assert k == size
    return out


def local_order(x, axis):
    me, levels = lax.axis_index(axis), bits_of(axis)
    y = x.reshape((2,) * len(levels) + (-1, x.shape[1]))
    for dim, bit in enumerate(levels):
        y = jnp.where((me & bit) != 0, jnp.flip(y, dim), y)
    return y.reshape(x.shape)


def up_half(x, gain, w_gate, w_up):
    xf = x.astype(f32)
    squares = jnp.sum(xf * xf, axis=1, keepdims=True)
    high = squares.astype(bf16).astype(f32)
    normed = (xf * gain.astype(f32)).astype(bf16)
    gate = jnp.dot(normed, w_gate, preferred_element_type=f32)
    up = jnp.dot(normed, w_up, preferred_element_type=f32)
    lane = lax.broadcasted_iota(jnp.int32, (x.shape[0], 128), 1)
    sq = jnp.where(lane == 0, high, jnp.where(lane == 1, squares - high, 0.0))
    return jnp.concatenate([gate, up, sq], axis=1)


def chain(x, layers):
    x = local_order(x, "ra")
    for gain, w_gate, w_up, w_down in layers:
        width = x.shape[1] * lax.axis_size("ra")
        ff = w_gate.shape[1]
        part = up_half(x, gain, w_gate, w_up)
        for bit in bits_of("ra"):
            half = part.shape[0] // 2
            got = yield part[half:].astype(bf16), "ra", bit
            part = part[:half] + got.astype(f32)
        total = part[:, 2 * ff : 2 * ff + 1] + part[:, 2 * ff + 1 : 2 * ff + 2]
        scale = lax.rsqrt(total / width + 1e-06)
        hidden = (jax.nn.silu(part[:, :ff] * scale) * (part[:, ff : 2 * ff] * scale)).astype(bf16)
        for bit in reversed(bits_of("ra")):
            got = yield hidden, "ra", bit
            hidden = jnp.concatenate([hidden, got], axis=0)
        branch = jnp.dot(hidden, w_down, preferred_element_type=f32)
        for bit in bits_of("cb"):
            got = yield branch.astype(bf16), "cb", bit
            branch = branch + got.astype(f32)
        x = (0.5 * x.astype(f32) + 0.5 * branch).astype(bf16)
    yield local_order(x, "ra")


def per_device(tokens, first_gain, first_gate, first_up, first_down, second_gain, second_gate, second_up, second_down):
    layers = ((first_gain, first_gate, first_up, first_down), (second_gain, second_gate, second_up, second_down))
    rows = tokens.shape[0] // CHUNKS
    chains = [chain(tokens[c * rows : (c + 1) * rows], layers) for c in range(CHUNKS)]
    arrived, last = [None] * CHUNKS, None
    while True:
        for c in range(CHUNKS):
            asked = chains[c].send(arrived[c])
            if isinstance(asked, tuple):
                payload, axis, bit = asked
                if last is not None:
                    payload, _ = lax.optimization_barrier((payload, last))
                last = payload
                arrived[c] = lax.ppermute(payload, axis, [(i, i ^ bit) for i in range(lax.axis_size(axis))])
            else:
                arrived[c] = asked
        if not isinstance(asked, tuple):
            return jnp.concatenate(arrived, axis=0)


def solution(mesh):
    placed = (
        P("grp", "ra"),
        P("ra"),
        P("ra", "cb"),
        P("ra", "cb"),
        P("cb", "ra"),
        P("ra"),
        P("ra", "cb"),
        P("ra", "cb"),
        P("cb", "ra"),
    )
    return jax.shard_map(
        per_device, mesh=mesh, in_specs=placed, out_specs=P("grp", "ra"), check_vma=False
    )
```

```python
import jax
import jax.numpy as jnp
from jax import lax
from jax.sharding import PartitionSpec as P

CHUNKS = 2
LAG_US = 6.0
COST_US = {'scatter': 11.0, 'gather': 8.5, 'core': 1.8, 'chip': 6.0}
bf16, f32 = jnp.bfloat16, jnp.float32


def bits_of(axis):
    size, out, k = lax.axis_size(axis), [], 1
    while k < size:
        out.append(k)
        k *= 2
    assert k == size
    return out


def rounds_of(axis, together):
    bits, out = bits_of(axis), []
    for at in range(0, len(bits), together):
        flips = [0]
        for bit in bits[at : at + together]:
            flips = [f | g for f in flips for g in (0, bit)]
        out.append(flips)
    return out


def local_order(x, axis):
    me, levels = lax.axis_index(axis), bits_of(axis)
    y = x.reshape((2,) * len(levels) + (-1, x.shape[1]))
    for dim, bit in enumerate(levels):
        y = jnp.where((me & bit) != 0, jnp.flip(y, dim), y)
    return y.reshape(x.shape)


def up_half(x, gain, w_gate, w_up):
    xf = x.astype(f32)
    squares = jnp.sum(xf * xf, axis=1, keepdims=True)
    high = squares.astype(bf16).astype(f32)
    normed = (xf * gain.astype(f32)).astype(bf16)
    gate = jnp.dot(normed, w_gate, preferred_element_type=f32)
    up = jnp.dot(normed, w_up, preferred_element_type=f32)
    lane = lax.broadcasted_iota(jnp.int32, (x.shape[0], 128), 1)
    sq = jnp.where(lane == 0, high, jnp.where(lane == 1, squares - high, 0.0))
    return jnp.concatenate([gate, up, sq], axis=1)


def chain(x, layers):
    x = local_order(x, "ra")
    for gain, w_gate, w_up, w_down in layers:
        width = x.shape[1] * lax.axis_size("ra")
        ff = w_gate.shape[1]
        part = up_half(x, gain, w_gate, w_up)
        for flips in rounds_of("ra", 2):
            rows = part.shape[0] // len(flips)
            blocks = [part[j * rows : (j + 1) * rows] for j in range(len(flips))]
            got = yield [(b.astype(bf16), "ra", f) for b, f in list(zip(blocks, flips))[1:]], "scatter"
            part = sum([g.astype(f32) for g in got], blocks[0])
        total = part[:, 2 * ff : 2 * ff + 1] + part[:, 2 * ff + 1 : 2 * ff + 2]
        scale = lax.rsqrt(total / width + 1e-06)
        hidden = (jax.nn.silu(part[:, :ff] * scale) * (part[:, ff : 2 * ff] * scale)).astype(bf16)
        for flips in reversed(rounds_of("ra", 2)):
            got = yield [(hidden, "ra", f) for f in flips[1:]], "gather"
            hidden = jnp.concatenate([hidden] + got, axis=0)
        branch = jnp.dot(hidden, w_down, preferred_element_type=f32)
        for bit in bits_of("cb"):
            (got,) = yield [(branch.astype(bf16), "cb", bit)], "core" if bit == 1 else "chip"
            branch = branch + got.astype(f32)
        x = (0.5 * x.astype(f32) + 0.5 * branch).astype(bf16)
    yield local_order(x, "ra")


def per_device(tokens, first_gain, first_gate, first_up, first_down, second_gain, second_gate, second_up, second_down):
    layers = ((first_gain, first_gate, first_up, first_down), (second_gain, second_gate, second_up, second_down))
    rows = tokens.shape[0] // CHUNKS
    chains = [chain(tokens[c * rows : (c + 1) * rows], layers) for c in range(CHUNKS)]
    arrived, last = [None] * CHUNKS, None
    clock = [c * LAG_US for c in range(CHUNKS)]
    running = list(range(CHUNKS))
    while running:
        c = min(running, key=lambda c: (clock[c], c))
        asked = chains[c].send(arrived[c])
        if isinstance(asked, tuple):
            asked, kind = asked
            clock[c] += COST_US[kind]
            payloads = [a[0] for a in asked]
            if last is not None:
                payloads = lax.optimization_barrier((*payloads, last))[:-1]
            last = payloads[0]
            arrived[c] = [
                lax.ppermute(p, axis, [(i, i ^ flip) for i in range(lax.axis_size(axis))])
                for p, (_, axis, flip) in zip(payloads, asked)
            ]
        else:
            arrived[c] = asked
            running.remove(c)
    return jnp.concatenate(arrived, axis=0)


def solution(mesh):
    placed = (
        P("grp", "ra"),
        P("ra"),
        P("ra", "cb"),
        P("ra", "cb"),
        P("cb", "ra"),
        P("ra"),
        P("ra", "cb"),
        P("ra", "cb"),
        P("cb", "ra"),
    )
    return jax.shard_map(
        per_device, mesh=mesh, in_specs=placed, out_specs=P("grp", "ra"), check_vma=False
    )
```
